32 devices in a mesh: sp: 8 (over z, x), tp: 4 (over y, core).
Axes of the slice: x: 2, y: 2, z: 4, core: 2. Of those that a mesh axis runs over, the one named last changes fastest.
Arguments:
- mixer_in: bfloat16 [2048, 2048], P('sp', 'tp'), may hold values from -6 to 6
- doc_ids: int32 [2048], P('sp'), may hold values from 0 to 3, never falling along the last dimension, each value on 1 to 1024 neighbouring positions
- mix_scale: float32 [2048], P('tp'), may hold values from 0.1 to 1.9
- out_proj: bfloat16 [2048, 2048], P('tp'), may hold values from -0.125 to 0.125
- residual: bfloat16 [2048, 2048], P('sp'), may hold values from -6 to 6
- mix_gain: float32 [2048], replicated, may hold values from 0.1 to 1.9
- expert_ids: int32 [2048, 2], P('sp'), may hold values from 0 to 7, all different within a row; in each aligned block of 256 rows (0 to 255, 256 to 511, ...) at most 128 rows name the same one
- expert_weight: float32 [2048, 2], P('sp'), may hold values from 0.2 to 1
- w_gate: bfloat16 [8, 2048, 5632], P('sp', None, 'tp'), may hold values from -0.125 to 0.125
- w_up: bfloat16 [8, 2048, 5632], P('sp', None, 'tp'), may hold values from -0.125 to 0.125
- w_down: bfloat16 [8, 5632, 2048], P('sp', 'tp'), may hold values from -0.078125 to 0.078125
- out_gain: float32 [2048], replicated, may hold values from 0.1 to 1.9
Outputs:
- layer_out: bfloat16 [2048, 2048], P('sp')
The draws below stay inside these ranges and needn't reach their ends.
Inputs may be any that keep to these rules, and one draw needn't show every extreme that they name: `doc_ids`: document numbers never fall along the tokens; a document has at most 1024 positions. `expert_ids`: A row's two experts differ. In each aligned block of 256 rows (the tokens of one index of sp) no expert is named by more than 128 rows; some block has an expert named by exactly 128 rows.
All inputs are finite; a program needn't handle non-finite values.
Results may differ from the reference program's by a relative error of at most 0.015.
Values may be sent and summed in bfloat16 or wider, within the bound.
A program may use at most 64 MiB of HBM per device.

```python
import math
import jax
import jax.numpy as jnp
import numpy as np
from jax import lax

D = 2048
FF = 5632
TOK_SP = 256
TOKENS = 2048
EXPERTS = 8
CAP = 128
FF_DEV = 1408
N_SP = 8
N_TP = 4


def block_scale(own_key, dims, pieces, smallest, top_value):
    def one(position, shards_of):
        draws = jax.random.uniform(jax.random.fold_in(jax.random.fold_in(own_key, 6), position), (shards_of,), jnp.float32, smallest / len(pieces), top_value / len(pieces))
        return jnp.repeat(jnp.exp(draws), dims[position] // shards_of).reshape((-1,) + (1,) * (len(dims) - position - 1))

    level = one(*pieces[0])
    for cut in pieces[1:]:
        level = level * one(*cut)
    return level


def profile(amount, total, limit, slope):
    weights = [(1 << 20) // math.isqrt(grade ** slope) + 1 for grade in range(2, amount + 1)]
    surplus, given = total - limit - (amount - 1), [1] * (amount - 1)
    while surplus > 0:
        free = [i for i in range(amount - 1) if given[i] < limit]
        mass, remaining = sum([weights[i] for i in free]), surplus
        for i in free:
            extra = min(limit - given[i], max(1, remaining * weights[i] // mass), surplus)
            given[i] = given[i] + extra
            surplus = surplus - extra
    return np.array([limit] + given)


def uneven_parts(rng, count, total, reach, lean):
    if count == 2:
        one = jax.random.randint(rng, (), max(1, total - reach), min(reach, total - 1) + 1)
        return jnp.stack([one, total - one])
    sizes = jnp.asarray(profile(count, total, reach, lean), jnp.int32)
    pairs = (count - 1) // 2
    donor, sink = sizes[1:1 + 2 * pairs:2], sizes[2:2 + 2 * pairs:2]
    room = jnp.minimum(donor - 1, reach - sink)
    moved = jax.random.randint(jax.random.fold_in(rng, 1), (pairs,), 0, 1 << 20) % (room + 1)
    sizes = sizes.at[1:1 + 2 * pairs:2].set(donor - moved).at[2:2 + 2 * pairs:2].set(sink + moved)
    return sizes[jax.random.permutation(jax.random.fold_in(rng, 2), count)]


def shared_out(key, own, number, rows, number_of, top, limit, slope):
    sequence = jax.random.permutation(key, number_of)
    packed, usual = shares(number_of, rows * top, limit, slope, True), shares(number_of, rows * top, limit, slope, False)
    places = jnp.arange(number_of)

    def named(sizes, offset_by):
        used = int((sizes > 0).sum())
        fixed = max(1, used // 4)
        moved = fixed + (places - fixed + offset_by * (used - fixed)) % max(1, number_of - fixed)
        return jnp.zeros((number_of,), jnp.int32).at[sequence[jnp.where(places < fixed, places, moved)]].set(jnp.asarray(sizes, jnp.int32))

    sizes = jnp.where(number % 4 == 0, named(packed, number // 4), named(usual, number - number // 4 - 1))
    mixed = jax.random.permutation(jax.random.fold_in(own, 3), number_of)
    giver, sink = mixed[0:number_of // 2 * 2:2], mixed[1:number_of // 2 * 2:2]
    margin = jnp.minimum(sizes[giver] - 1, limit - sizes[sink]) // 2
    margin = jnp.where((giver == sequence[0]) | (sink == sequence[0]) | (sizes[sink] == 0), 0, jnp.maximum(margin, 0))
    moved = jax.random.randint(jax.random.fold_in(own, 4), (number_of // 2,), 0, 1 << 20) % (margin + 1)
    sizes = sizes.at[giver].add(-moved).at[sink].add(moved)
    members = jnp.searchsorted(jnp.cumsum(sizes), jnp.arange(rows * top), side="right").astype(jnp.int32)
    table = members.reshape(top, rows).T
    table = table[jax.random.permutation(jax.random.fold_in(own, 1), rows)]
    offset_by = jax.random.randint(jax.random.fold_in(own, 2), (rows, 1), 0, top)
    return jnp.take_along_axis(table, (jnp.arange(top)[None, :] + offset_by) % top, axis=1)


def shares(number_of, total, bound, skew, full):
    portions = [(1 << 20) // math.isqrt(rank ** skew) + 1 for rank in range(1, number_of + 1)]
    largest = bound if full else min(bound, max(-(-total // number_of), total * portions[0] // sum(portions)))
    least = 1 if total - largest >= number_of - 1 else 0
    holding, rest = [largest] + [least] * (number_of - 1), total - largest - least * (number_of - 1)
    while rest > 0:
        movable = [i for i in range(1, number_of) if holding[i] < largest] or [i for i in range(1, number_of) if holding[i] < bound]
        whole, left = sum([portions[i] for i in movable]), rest
        for i in movable:
            extra = min(bound - holding[i], max(1, left * portions[i] // whole), rest)
            holding[i] = holding[i] + extra
            rest = rest - extra
    return np.array(holding)


def scatter_about(stream_key, shape, scale, bound, cuts=(), held_as=jnp.bfloat16):
    factor_of = block_scale(stream_key, shape, cuts, -0.22, 0.18) if cuts else 1.0
    drawn = jax.random.normal(stream_key, shape, jnp.float32) * scale * factor_of
    return jnp.minimum(jnp.maximum(drawn, -bound), bound).astype(held_as)


def setup_inputs(seed: int = 0) -> dict:
    seeds = jax.random.split(jax.random.key(seed), 13)
    mixer_in = scatter_about(seeds[0], (TOKENS, D), 1.0, 6.0, ((0, 8), (1, 4)))
    doc_ids = jnp.searchsorted(jnp.cumsum(uneven_parts(seeds[1], N_SP // 2, TOKENS, 4 * TOK_SP, 1)), jnp.arange(TOKENS), side="right").astype(jnp.int32)
    mix_scale = jnp.clip(1.0 + 0.18 * jax.random.normal(seeds[2], (D,), jnp.float32), 0.1, 1.9)
    out_proj = scatter_about(seeds[3], (D, D), D ** -0.5, 0.125, ((0, 4),))
    residual = scatter_about(seeds[4], (TOKENS, D), 1.0, 6.0, ((0, 8),))
    mix_gain = jnp.clip(1.0 + 0.18 * jax.random.normal(seeds[5], (D,), jnp.float32), 0.1, 1.9)
    expert_ids_keys = jax.random.split(jax.random.fold_in(seeds[6], 1), TOKENS // TOK_SP)
    expert_ids_turns = jax.random.permutation(jax.random.fold_in(seeds[6], 3), TOKENS // TOK_SP)
    expert_ids = jax.vmap(lambda own, number: shared_out(jax.random.fold_in(seeds[6], 2), own, number, TOK_SP, EXPERTS, 2, CAP, 2))(expert_ids_keys, expert_ids_turns).reshape((TOKENS, 2))
    expert_weight = jnp.clip(0.2 + 0.8 * jax.random.uniform(seeds[7], (TOKENS, 2), jnp.float32) ** block_scale(seeds[7], (TOKENS, 2), ((0, 8),), -0.2, 0.2), 0.2, 1.0)
    w_gate = scatter_about(seeds[8], (EXPERTS, D, FF), D ** -0.5, 0.125, ((0, 8), (2, 4)))
    w_up = scatter_about(seeds[9], (EXPERTS, D, FF), D ** -0.5, 0.125, ((0, 8), (2, 4)))
    w_down = scatter_about(seeds[10], (EXPERTS, FF, D), FF ** -0.5, 0.078125, ((0, 8), (1, 4)))
    out_gain = jnp.clip(1.0 + 0.18 * jax.random.normal(seeds[11], (D,), jnp.float32), 0.1, 1.9)
    return dict(mixer_in=mixer_in, doc_ids=doc_ids, mix_scale=mix_scale, out_proj=out_proj, residual=residual, mix_gain=mix_gain, expert_ids=expert_ids, expert_weight=expert_weight, w_gate=w_gate, w_up=w_up, w_down=w_down, out_gain=out_gain)


alpha_res = 1.4142135623730951
norm_eps = 1e-05
pool_reach = 15

def layer_norm(summed, norm_gain):
    row_mean = lax.optimization_barrier(jnp.mean(summed, axis=-1, keepdims=True))
    centred = summed - row_mean
    row_var = lax.optimization_barrier(jnp.mean(centred * centred, axis=-1, keepdims=True))
    return centred * lax.rsqrt(row_var + norm_eps) * norm_gain

def pair_slots(pair_ids, experts):
    flat_ids = pair_ids.reshape(-1)
    onehot = (flat_ids[:, None] == jnp.arange(experts, dtype=jnp.int32)[None, :]).astype(jnp.int32)
    before = jnp.cumsum(onehot, axis=0) - onehot
    return lax.optimization_barrier(jnp.sum(before * onehot, axis=1)).reshape(pair_ids.shape).astype(jnp.int32)

def reference(mixer_in, doc_ids, mix_scale, out_proj, residual, mix_gain, expert_ids, expert_weight, w_gate, w_up, w_down, out_gain):
    tokens, features = mixer_in.shape
    values = mixer_in.astype(jnp.float32)
    positions = jnp.arange(tokens, dtype=jnp.int32)
    channel = jnp.arange(features, dtype=jnp.int32)
    window = jnp.left_shift(jnp.int32(2), (channel // (features // 4)).astype(jnp.int32))
    window_sum = jnp.zeros((tokens, features), jnp.float32)
    window_count = jnp.zeros((tokens, features), jnp.float32)
    for lag_step in range(pool_reach + 1):
        shifted = jnp.concatenate([jnp.zeros((lag_step, features), jnp.float32), values[:tokens - lag_step]], axis=0)
        shifted_doc = jnp.concatenate([jnp.full((lag_step,), -1, jnp.int32), doc_ids[:tokens - lag_step]], axis=0)
        same_doc = (shifted_doc == doc_ids) & (positions >= lag_step)
        in_window = (same_doc[:, None] & (lag_step < window)[None, :]).astype(jnp.float32)
        window_sum = window_sum + in_window * shifted
        window_count = window_count + in_window
    mixed_rows = ((window_sum / window_count - values) * mix_scale).astype(jnp.bfloat16)
    projected = jnp.dot(mixed_rows, out_proj, preferred_element_type=jnp.float32)
    normed = layer_norm(alpha_res * residual.astype(jnp.float32) + projected, mix_gain).astype(jnp.bfloat16)
    experts = w_gate.shape[0]
    blocks = N_SP
    block_rows = tokens // blocks
    capacity = CAP
    ids_blocks = expert_ids.reshape(blocks, block_rows, 2)
    ranks = jax.vmap(lambda pair_ids: pair_slots(pair_ids, experts))(ids_blocks)
    target = (ids_blocks * capacity + ranks).astype(jnp.int32)
    block_index = jnp.broadcast_to(jnp.arange(blocks, dtype=jnp.int32)[:, None, None], target.shape)
    row_index = jnp.broadcast_to(jnp.arange(block_rows, dtype=jnp.int32)[None, :, None], target.shape)
    slot_row = jnp.full((blocks, experts * capacity), block_rows, jnp.int32).at[block_index, target].set(row_index)
    normed_blocks = jnp.concatenate([normed.reshape(blocks, block_rows, features), jnp.zeros((blocks, 1, features), jnp.bfloat16)], axis=1)
    expert_in = jnp.take_along_axis(normed_blocks, slot_row[:, :, None], axis=1)
    expert_in = expert_in.reshape(blocks, experts, capacity, features).transpose(1, 0, 2, 3)

    def one_expert(inputs):
        rows_in, gate_w, up_w, down_w = inputs
        flat_in = rows_in.reshape(-1, features)
        gate_pre = jnp.dot(flat_in, gate_w, preferred_element_type=jnp.float32)
        upper = jnp.dot(flat_in, up_w, preferred_element_type=jnp.float32)
        hidden = (jax.nn.silu(gate_pre) * upper).astype(jnp.bfloat16)
        split_hidden = hidden.reshape(-1, N_TP, FF_DEV).astype(jnp.float32)
        split_down = down_w.reshape(N_TP, FF_DEV, features).astype(jnp.float32)
        parts = jnp.einsum('rjf,jfd->jrd', split_hidden, split_down).astype(jnp.bfloat16)
        return lax.optimization_barrier(jnp.sum(parts.astype(jnp.float32), axis=0)).reshape(blocks, capacity, features)
    outputs = lax.map(one_expert, (expert_in, w_gate, w_up, w_down))
    outputs = outputs.transpose(1, 0, 2, 3).reshape(blocks, experts * capacity, features)
    picked = jnp.take_along_axis(outputs, target.reshape(blocks, -1)[:, :, None], axis=1)
    picked = picked.reshape(blocks, block_rows, 2, features)
    routed = lax.optimization_barrier(jnp.sum(picked * expert_weight.reshape(blocks, block_rows, 2)[..., None], axis=2)).reshape(tokens, features)
    return layer_norm(alpha_res * normed.astype(jnp.float32) + routed, out_gain).astype(jnp.bfloat16)
```

```python
import functools

import jax
import jax.numpy as jnp
from jax import lax
from jax.experimental import pallas as pl
from jax.experimental.pallas import tpu as pltpu
from jax.sharding import PartitionSpec as P

MESH = pl.DeviceIdType.MESH
DMA = pltpu.SemaphoreType.DMA
f32 = jnp.float32
bf16 = jnp.bfloat16

alpha_res = 1.4142135623730951
norm_eps = 1e-05
pool_reach = 15


def passed_along(value, axis, steps):
    count = lax.axis_size(axis)
    initial, last = (max(0, -steps), min(count, count - steps))
    return lax.ppermute(value, axis, [(source, source + steps) for source in range(initial, last)])


def layer_norm(summed, norm_gain):
    row_mean = jnp.mean(summed, axis=-1, keepdims=True)
    centred = summed - row_mean
    row_var = jnp.mean(centred * centred, axis=-1, keepdims=True)
    return centred * lax.rsqrt(row_var + norm_eps) * norm_gain


def pair_slots(pair_ids, experts):
    flat_ids = pair_ids.reshape(-1)
    onehot = (flat_ids[:, None] == jnp.arange(experts, dtype=jnp.int32)[None, :]).astype(jnp.int32)
    before = jnp.cumsum(onehot, axis=0) - onehot
    return jnp.sum(before * onehot, axis=1).reshape(pair_ids.shape)


def wrapped(value, count):
    return lax.rem(value + 2 * count, count)


def place(n_tp):
    me = lax.axis_index("tp")
    return lax.div(me, 2), lax.rem(me, 2)


def sent(src, dst, send_sem, recv_sem, device):
    return pltpu.make_async_remote_copy(
        src_ref=src,
        dst_ref=dst,
        send_sem=send_sem,
        recv_sem=recv_sem,
        device_id=device,
        device_id_type=MESH,
    )


def greet(n_sp, n_tp):
    y, core = place(n_tp)
    n_y = n_tp // 2
    barrier = pltpu.get_barrier_semaphore()
    pl.semaphore_signal(
        barrier, inc=1, device_id={"tp": y * 2 + 1 - core}, device_id_type=MESH
    )
    for j in range(1, n_y):
        pl.semaphore_signal(
            barrier, inc=1, device_id={"tp": wrapped(y + j, n_y) * 2 + core}, device_id_type=MESH
        )
    if n_sp > 1:
        me = lax.axis_index("sp")

        def tell(k, carry):
            pl.semaphore_signal(
                barrier, inc=1, device_id={"sp": wrapped(me + k, n_sp)}, device_id_type=MESH
            )
            return carry

        lax.fori_loop(1, n_sp, tell, 0)
    pl.semaphore_wait(barrier, n_y + n_sp - 1)


def spread(n_y, y, core, part, sems):
    send_y, recv_y, send_c, recv_c = sems
    other = {"tp": y * 2 + 1 - core}
    own = part(y, core)
    along = []
    for j in range(1, n_y):
        copy = sent(
            own, own, send_y.at[j], recv_y.at[j], {"tp": wrapped(y + j, n_y) * 2 + core}
        )
        copy.start()
        along.append(copy)
    across = [sent(own, own, send_c.at[0], recv_c.at[0], other)]
    across[0].start()
    for j in range(1, n_y):
        came = part(wrapped(y - j, n_y), core)
        sent(came, came, send_y.at[j], recv_y.at[j], other).wait_recv()
        copy = sent(came, came, send_c.at[j], recv_c.at[j], other)
        copy.start()
        across.append(copy)
    for j in range(n_y):
        came = part(wrapped(y - j, n_y), 1 - core)
        sent(came, came, send_c.at[j], recv_c.at[j], other).wait_recv()
    for copy in along + across:
        copy.wait_send()


def project_kernel(
    n_tp, proj, residual, gain, normed, recv_a, send_b, recv_b, sa, ra, sb, rb, sy, ry, sc, rc
):
    y, core = place(n_tp)
    n_y = n_tp // 2
    share = proj.shape[0] // n_tp
    other = {"tp": y * 2 + 1 - core}

    def rows(y_of, core_of):
        return pl.ds(pl.multiple_of((core_of * n_y + y_of) * share, share), share)

    greet(1, n_tp)
    halves = {}
    for j in list(range(1, n_y)) + [0]:
        y_to = wrapped(y + j, n_y)
        halves[j] = sent(
            proj.at[rows(y_to, 1 - core)], recv_a.at[j], sa.at[j], ra.at[j], other
        )
        halves[j].start()
    along = []
    for j in range(1, n_y):
        y_to = wrapped(y + j, n_y)
        halves[j].wait_recv()
        send_b[j] = (proj[rows(y_to, core), :].astype(f32) + recv_a[j].astype(f32)).astype(bf16)
        copy = sent(
            send_b.at[j], recv_b.at[j], sb.at[j], rb.at[j], {"tp": y_to * 2 + core}
        )
        copy.start()
        along.append(copy)
    halves[0].wait_recv()
    summed = proj[rows(y, core), :].astype(f32) + recv_a[0].astype(f32)
    summed = summed + alpha_res * residual[rows(y, core), :].astype(f32)
    for j in range(1, n_y):
        along[j - 1].wait_recv()
        summed = summed + recv_b[j].astype(f32)
    normed[rows(y, core), :] = layer_norm(summed, gain[...]).astype(bf16)
    spread(n_y, y, core, lambda a, b: normed.at[rows(a, b)], (sy, ry, sc, rc))
    for copy in list(halves.values()) + along:
        copy.wait_send()


def dispatch_kernel(
    n_sp, n_tp, select, normed, x, send, s1, r1, s2, r2, s3, r3
):
    y, core = place(n_tp)
    n_y = n_tp // 2
    me = lax.axis_index("sp")
    cap = select.shape[0] // n_sp
    width = normed.shape[1] // n_tp
    other = {"tp": y * 2 + 1 - core}

    def cols(y_of, core_of):
        return pl.ds(pl.multiple_of((core_of * n_y + y_of) * width, width), width)

    def rows(block):
        return pl.ds(pl.multiple_of(block * cap, cap), cap)

    own = cols(y, core)
    greet(n_sp, n_tp)

    def picked(block):
        return jnp.dot(
            select[rows(block), :], normed[:, own], preferred_element_type=f32
        ).astype(bf16)

    def first(k):
        to = wrapped(me + k, n_sp)
        return sent(send.at[rows(to)], x.at[rows(me), own], s1.at[k], r1.at[k], {"sp": to})

    def along(k, j):
        piece = x.at[rows(wrapped(me - k, n_sp)), own]
        return sent(piece, piece, s2.at[j, k], r2.at[j, k], {"tp": wrapped(y + j, n_y) * 2 + core})

    def across(k, j, core_of):
        piece = x.at[rows(wrapped(me - k, n_sp)), cols(wrapped(y - j, n_y), core_of)]
        return sent(piece, piece, s3.at[j, k], r3.at[j, k], other)

    def start_first(k, carry):
        to = wrapped(me + k, n_sp)
        send[rows(to), :] = picked(to)
        first(k).start()
        return carry

    lax.fori_loop(1, n_sp, start_first, 0)
    x[rows(me), own] = picked(me)

    def forward(k):
        for j in range(1, n_y):
            along(k, j).start()
        across(k, 0, core).start()

    def second(k):
        for j in range(1, n_y):
            came = x.at[rows(wrapped(me - k, n_sp)), cols(wrapped(y - j, n_y), core)]
            sent(came, came, s2.at[j, k], r2.at[j, k], other).wait_recv()
            across(k, j, core).start()

    forward(0)

    def body(k, carry):
        came = x.at[rows(wrapped(me - k, n_sp)), own]
        sent(came, came, s1.at[k], r1.at[k], other).wait_recv()
        forward(k)
        second(k - 1)
        return carry

    lax.fori_loop(1, n_sp, body, 0)
    second(n_sp - 1)

    def finish(k, carry):
        for j in range(n_y):
            across(k, j, 1 - core).wait_recv()
            across(k, j, core).wait_send()
        for j in range(1, n_y):
            along(k, j).wait_send()
        return carry

    lax.fori_loop(0, n_sp, finish, 0)

    def finish_first(k, carry):
        first(k).wait_send()
        return carry

    lax.fori_loop(1, n_sp, finish_first, 0)


def combine_kernel(
    n_sp, n_tp, partial, mix_hi, mix_lo, normed, gain, out,
    recv_a, send_b, recv_b, send_c, recv_c, routed,
    sa, ra, sb, rb, s1, r1, sy, ry, sc, rc,
):
    y, core = place(n_tp)
    n_y = n_tp // 2
    me = lax.axis_index("sp")
    cap = partial.shape[0] // n_sp
    features = partial.shape[1]
    width, half = features // n_tp, features // 2
    other = {"tp": y * 2 + 1 - core}

    def cols(y_of, core_of):
        return pl.ds(pl.multiple_of((core_of * n_y + y_of) * width, width), width)

    def sub(y_of):
        return pl.ds(pl.multiple_of(y_of * width, width), width)

    def rows(block):
        return pl.ds(pl.multiple_of(block * cap, cap), cap)

    def block_of(k):
        return wrapped(me + k + 1, n_sp)

    greet(n_sp, n_tp)

    def across(k):
        at = rows(block_of(k))
        far = pl.ds(pl.multiple_of((1 - core) * half, half), half)
        return sent(partial.at[at, far], recv_a.at[at], sa.at[k], ra.at[k], other)

    def along(k, j):
        at = rows(block_of(k))
        return sent(
            send_b.at[j, at], recv_b.at[j, at], sb.at[j, k], rb.at[j, k],
            {"tp": wrapped(y + j, n_y) * 2 + core},
        )

    def home(k):
        to = block_of(k)
        return sent(send_c.at[rows(to)], recv_c.at[rows(me)], s1.at[k], r1.at[k], {"sp": to})

    def start_a(k, carry):
        across(k).start()
        return carry

    lax.fori_loop(0, n_sp, start_a, 0)

    def start_b(k, carry):
        across(k).wait_recv()
        at = rows(block_of(k))
        for j in range(1, n_y):
            y_to = wrapped(y + j, n_y)
            send_b[j, at, :] = (
                partial[at, cols(y_to, core)].astype(f32) + recv_a[at, sub(y_to)].astype(f32)
            ).astype(bf16)
            along(k, j).start()
        return carry

    lax.fori_loop(0, n_sp, start_b, 0)

    def total(k):
        at = rows(block_of(k))
        summed = partial[at, cols(y, core)].astype(f32) + recv_a[at, sub(y)].astype(f32)
        for j in range(1, n_y):
            along(k, j).wait_recv()
            summed = summed + recv_b[j, at, :].astype(f32)
        return summed.astype(bf16)

    def start_c(k, carry):
        summed = total(k)
        send_c[rows(block_of(k)), :] = summed
        home(k).start()
        return carry

    lax.fori_loop(0, n_sp - 1, start_c, 0)
    recv_c[rows(me), :] = total(n_sp - 1)

    def finish_c(k, carry):
        came = recv_c.at[rows(wrapped(me - k - 1, n_sp))]
        sent(came, came, s1.at[k], r1.at[k], other).wait_recv()
        home(k).wait_send()
        return carry

    lax.fori_loop(0, n_sp - 1, finish_c, 0)
    routed[:, cols(y, core)] = (
        jnp.dot(mix_hi[...], recv_c[...], preferred_element_type=f32)
        + jnp.dot(mix_lo[...], recv_c[...], preferred_element_type=f32)
    ).astype(bf16)
    spread(n_y, y, core, lambda a, b: routed.at[:, cols(a, b)], (sy, ry, sc, rc))
    step = 64

    def norm(i, carry):
        at = pl.ds(pl.multiple_of(i * step, step), step)
        summed = alpha_res * normed[at, :].astype(f32) + routed[at, :].astype(f32)
        out[at, :] = layer_norm(summed, gain[...]).astype(bf16)
        return carry

    lax.fori_loop(0, out.shape[0] // step, norm, 0)

    def finish(k, carry):
        across(k).wait_send()
        for j in range(1, n_y):
            along(k, j).wait_send()
        return carry

    lax.fori_loop(0, n_sp, finish, 0)


def called(kernel, args, shape, scratch, number):
    return pl.pallas_call(
        kernel,
        out_shape=jax.ShapeDtypeStruct(shape, bf16),
        in_specs=[pl.BlockSpec(memory_space=pltpu.VMEM)] * len(args),
        out_specs=pl.BlockSpec(memory_space=pltpu.VMEM),
        scratch_shapes=scratch,
        compiler_params=pltpu.CompilerParams(
            collective_id=number, has_side_effects=True, vmem_limit_bytes=60 * 1024 * 1024
        ),
    )(*args)


def spread_sems(n_y):
    return [DMA((n_y,))] * 4


def project(proj, residual, gain, n_tp):
    rows, features = proj.shape
    n_y, share = n_tp // 2, rows // n_tp
    piece = pltpu.VMEM((n_y, share, features), bf16)
    return called(
        functools.partial(project_kernel, n_tp),
        (proj, residual, gain.reshape(1, features)),
        (rows, features),
        [piece] * 3 + [DMA((n_y,))] * 4 + spread_sems(n_y),
        0,
    )


def dispatch(select, normed, n_sp, n_tp):
    slots, features = select.shape[0], normed.shape[1]
    n_y = n_tp // 2
    return called(
        functools.partial(dispatch_kernel, n_sp, n_tp),
        (select, normed),
        (slots, features),
        [pltpu.VMEM((slots, features // n_tp), bf16)]
        + [DMA((n_sp,))] * 2
        + [DMA((n_y, n_sp))] * 4,
        1,
    )


def combine(partial, mix_hi, mix_lo, normed, gain, n_sp, n_tp):
    slots, features = partial.shape
    rows = normed.shape[0]
    n_y, width = n_tp // 2, features // n_tp
    return called(
        functools.partial(combine_kernel, n_sp, n_tp),
        (partial, mix_hi, mix_lo, normed, gain.reshape(1, features)),
        (rows, features),
        [
            pltpu.VMEM((slots, features // 2), bf16),
            pltpu.VMEM((n_y, slots, width), bf16),
            pltpu.VMEM((n_y, slots, width), bf16),
            pltpu.VMEM((slots, width), bf16),
            pltpu.VMEM((slots, width), bf16),
            pltpu.VMEM((rows, features), bf16),
        ]
        + [DMA((n_sp,))] * 2
        + [DMA((n_y, n_sp))] * 2
        + [DMA((n_sp,))] * 2
        + spread_sems(n_y),
        2,
    )


def shards(
    mixer_in,
    doc_ids,
    mix_scale,
    out_proj,
    residual,
    mix_gain,
    expert_ids,
    expert_weight,
    w_gate,
    w_up,
    w_down,
    out_gain,
):
    tok_rows, chan_cols = mixer_in.shape
    features = mix_gain.shape[0]
    tail_rows = (mixer_in[tok_rows - pool_reach :], doc_ids[tok_rows - pool_reach :])
    before_vals, before_doc = passed_along((tail_rows[0], tail_rows[1]), "sp", 1)
    extended = jnp.concatenate([before_vals, mixer_in], axis=0).astype(jnp.float32)
    extended_doc = jnp.concatenate([before_doc, doc_ids], axis=0)
    positions = lax.axis_index("sp") * tok_rows + jnp.arange(tok_rows, dtype=jnp.int32)
    channel = lax.axis_index("tp") * chan_cols + jnp.arange(chan_cols, dtype=jnp.int32)
    window = jnp.left_shift(jnp.int32(2), channel // (features // 4))
    window_sum = jnp.zeros((tok_rows, chan_cols), jnp.float32)
    window_count = jnp.zeros((tok_rows, chan_cols), jnp.float32)
    for lag_step in range(pool_reach + 1):
        shifted = extended[pool_reach - lag_step : pool_reach - lag_step + tok_rows]
        same_doc = (
            extended_doc[pool_reach - lag_step : pool_reach - lag_step + tok_rows] == doc_ids
        ) & (positions >= lag_step)
        in_window = (same_doc[:, None] & (lag_step < window)[None, :]).astype(jnp.float32)
        window_sum = window_sum + in_window * shifted
        window_count = window_count + in_window
    mixed_rows = ((window_sum / window_count - extended[pool_reach:]) * mix_scale).astype(
        jnp.bfloat16
    )
    n_sp, n_tp = lax.axis_size("sp"), lax.axis_size("tp")
    product = jnp.dot(mixed_rows, out_proj, preferred_element_type=f32).astype(bf16)
    experts = n_sp
    capacity = 4 * tok_rows // experts
    ranks = pair_slots(expert_ids, experts)
    target = expert_ids * capacity + ranks
    slot_ids = jnp.arange(experts * capacity, dtype=jnp.int32)
    select = (
        (target[None, :, 0] == slot_ids[:, None]) | (target[None, :, 1] == slot_ids[:, None])
    ).astype(bf16)
    mix = jnp.sum(
        jnp.where(target[:, :, None] == slot_ids[None, None, :], expert_weight[:, :, None], 0.0),
        axis=1,
    )
    mix_hi = lax.reduce_precision(mix, 8, 7)
    mix_lo = (mix - mix_hi).astype(bf16)
    mix_hi = mix_hi.astype(bf16)
    normed = project(product, residual, mix_gain, n_tp)
    flat_in = dispatch(select, normed, n_sp, n_tp)
    gate_pre = jnp.dot(flat_in, w_gate[0], preferred_element_type=f32)
    upper = jnp.dot(flat_in, w_up[0], preferred_element_type=f32)
    hidden = (jax.nn.silu(gate_pre) * upper).astype(bf16)
    partial_value = jnp.dot(hidden, w_down[0], preferred_element_type=f32).astype(bf16)
    return combine(partial_value, mix_hi, mix_lo, normed, out_gain, n_sp, n_tp)


def solution(mesh):
    placed = (
        P("sp", "tp"),
        P("sp"),
        P("tp"),
        P("tp", None),
        P("sp", None),
        P(),
        P("sp", None),
        P("sp", None),
        P("sp", None, "tp"),
        P("sp", None, "tp"),
        P("sp", "tp", None),
        P(),
    )
    return jax.shard_map(
        shards, mesh=mesh, in_specs=placed, out_specs=P("sp", None), check_vma=False
    )
```

```python
import functools

import jax
import jax.numpy as jnp
from jax import lax
from jax.experimental import pallas as pl
from jax.experimental.pallas import tpu as pltpu
from jax.sharding import PartitionSpec as P

MESH = pl.DeviceIdType.MESH
DMA = pltpu.SemaphoreType.DMA
f32 = jnp.float32
bf16 = jnp.bfloat16

alpha_res = 1.4142135623730951
norm_eps = 1e-05
pool_reach = 15


def passed_along(value, axis, steps):
    count = lax.axis_size(axis)
    initial, last = (max(0, -steps), min(count, count - steps))
    return lax.ppermute(value, axis, [(source, source + steps) for source in range(initial, last)])


def layer_norm(summed, norm_gain):
    row_mean = jnp.mean(summed, axis=-1, keepdims=True)
    centred = summed - row_mean
    row_var = jnp.mean(centred * centred, axis=-1, keepdims=True)
    return centred * lax.rsqrt(row_var + norm_eps) * norm_gain


def pair_slots(pair_ids, experts):
    flat_ids = pair_ids.reshape(-1)
    onehot = (flat_ids[:, None] == jnp.arange(experts, dtype=jnp.int32)[None, :]).astype(jnp.int32)
    before = jnp.cumsum(onehot, axis=0) - onehot
    return jnp.sum(before * onehot, axis=1).reshape(pair_ids.shape)


def wrapped(value, count):
    return lax.rem(value + 2 * count, count)


def place(n_tp):
    me = lax.axis_index("tp")
    return lax.div(me, 2), lax.rem(me, 2)


def sent(src, dst, send_sem, recv_sem, device):
    return pltpu.make_async_remote_copy(
        src_ref=src,
        dst_ref=dst,
        send_sem=send_sem,
        recv_sem=recv_sem,
        device_id=device,
        device_id_type=MESH,
    )


def greet(n_sp, n_tp):
    y, core = place(n_tp)
    n_y = n_tp // 2
    barrier = pltpu.get_barrier_semaphore()
    pl.semaphore_signal(
        barrier, inc=1, device_id={"tp": y * 2 + 1 - core}, device_id_type=MESH
    )
    for j in range(1, n_y):
        pl.semaphore_signal(
            barrier, inc=1, device_id={"tp": wrapped(y + j, n_y) * 2 + core}, device_id_type=MESH
        )
    if n_sp > 1:
        me = lax.axis_index("sp")

        def tell(k, carry):
            pl.semaphore_signal(
                barrier, inc=1, device_id={"sp": wrapped(me + k, n_sp)}, device_id_type=MESH
            )
            return carry

        lax.fori_loop(1, n_sp, tell, 0)
    pl.semaphore_wait(barrier, n_y + n_sp - 1)


def spread(n_y, y, core, part, sems):
    send_y, recv_y, send_c, recv_c = sems
    other = {"tp": y * 2 + 1 - core}
    own = part(y, core)
    along = []
    for j in range(1, n_y):
        copy = sent(
            own, own, send_y.at[j], recv_y.at[j], {"tp": wrapped(y + j, n_y) * 2 + core}
        )
        copy.start()
        along.append(copy)
    across = [sent(own, own, send_c.at[0], recv_c.at[0], other)]
    across[0].start()
    for j in range(1, n_y):
        came = part(wrapped(y - j, n_y), core)
        sent(came, came, send_y.at[j], recv_y.at[j], other).wait_recv()
        copy = sent(came, came, send_c.at[j], recv_c.at[j], other)
        copy.start()
        across.append(copy)
    for j in range(n_y):
        came = part(wrapped(y - j, n_y), 1 - core)
        sent(came, came, send_c.at[j], recv_c.at[j], other).wait_recv()
    for copy in along + across:
        copy.wait_send()


def project_kernel(
    n_tp, proj, residual, gain, normed, recv_a, send_b, recv_b, sa, ra, sb, rb, sy, ry, sc, rc
):
    y, core = place(n_tp)
    n_y = n_tp // 2
    share = proj.shape[0] // n_tp
    other = {"tp": y * 2 + 1 - core}

    def rows(y_of, core_of):
        return pl.ds(pl.multiple_of((core_of * n_y + y_of) * share, share), share)

    greet(1, n_tp)
    halves = {}
    for j in list(range(1, n_y)) + [0]:
        y_to = wrapped(y + j, n_y)
        halves[j] = sent(
            proj.at[rows(y_to, 1 - core)], recv_a.at[j], sa.at[j], ra.at[j], other
        )
        halves[j].start()
    along = []
    for j in range(1, n_y):
        y_to = wrapped(y + j, n_y)
        halves[j].wait_recv()
        send_b[j] = (proj[rows(y_to, core), :].astype(f32) + recv_a[j].astype(f32)).astype(bf16)
        copy = sent(
            send_b.at[j], recv_b.at[j], sb.at[j], rb.at[j], {"tp": y_to * 2 + core}
        )
        copy.start()
        along.append(copy)
    halves[0].wait_recv()
    summed = proj[rows(y, core), :].astype(f32) + recv_a[0].astype(f32)
    summed = summed + alpha_res * residual[rows(y, core), :].astype(f32)
    for j in range(1, n_y):
        along[j - 1].wait_recv()
        summed = summed + recv_b[j].astype(f32)
    normed[rows(y, core), :] = layer_norm(summed, gain[...]).astype(bf16)
    spread(n_y, y, core, lambda a, b: normed.at[rows(a, b)], (sy, ry, sc, rc))
    for copy in list(halves.values()) + along:
        copy.wait_send()


def experts_kernel(
    n_sp, n_tp, select, normed, w_gate, w_up, w_down, mix_hi, mix_lo, gain, out,
    x, send, gate_v, up_v, down_v, partial, recv_a, send_b, recv_b, send_c, recv_c, routed,
    sw, s1, r1, s2, r2, s3, r3, sa, ra, sb, rb, s4, r4, sy, ry, sc, rc,
):
    y, core = place(n_tp)
    n_y = n_tp // 2
    me = lax.axis_index("sp")
    cap = select.shape[0] // n_sp
    features = normed.shape[1]
    width, half = features // n_tp, features // 2
    per = max(1, min(n_sp, 256 // cap))
    chunks = n_sp // per
    other = {"tp": y * 2 + 1 - core}

    def peer(k, sign):
        outer = wrapped(lax.div(me, 2) + sign * lax.div(k, 2), n_sp // 2)
        return outer * 2 + wrapped(lax.rem(me, 2) + sign * lax.rem(k, 2), 2)

    def cols(y_of, core_of):
        return pl.ds(pl.multiple_of((core_of * n_y + y_of) * width, width), width)

    def sub(y_of):
        return pl.ds(pl.multiple_of(y_of * width, width), width)

    def rows(block):
        return pl.ds(pl.multiple_of(block * cap, cap), cap)

    def along_tp(j):
        return {"tp": wrapped(y + j, n_y) * 2 + core}

    own = cols(y, core)
    loads = [
        pltpu.make_async_copy(source.at[0], held, sw.at[n])
        for n, (source, held) in enumerate(((w_gate, gate_v), (w_up, up_v), (w_down, down_v)))
    ]
    for load in loads:
        load.start()
    greet(n_sp, n_tp)

    def first(k):
        to = peer(k, 1)
        return sent(send.at[rows(k)], x.at[rows(k), own], s1.at[k], r1.at[k], {"sp": to})

    def along(k, j):
        piece = x.at[rows(k), own]
        return sent(piece, piece, s2.at[j, k], r2.at[j, k], along_tp(j))

    def across(k, j, core_of):
        piece = x.at[rows(k), cols(wrapped(y - j, n_y), core_of)]
        return sent(piece, piece, s3.at[j, k], r3.at[j, k], other)

    def start_first(k, carry):
        send[rows(k), :] = jnp.dot(
            select[rows(peer(k, 1)), :], normed[:, own], preferred_element_type=f32
        ).astype(bf16)
        first(k).start()
        return carry

    lax.fori_loop(1, n_sp, start_first, 0)
    x[rows(0), :] = jnp.dot(
        select[rows(me), :], normed[...], preferred_element_type=f32
    ).astype(bf16)

    def hop_one(i):
        def body(k, carry):
            first(k).wait_recv()
            for j in range(1, n_y):
                along(k, j).start()
            across(k, 0, core).start()
            return carry

        lax.fori_loop(jnp.maximum(i * per, 1), i * per + per, body, 0)

    def hop_two(i):
        def body(k, carry):
            for j in range(1, n_y):
                came = x.at[rows(k), cols(wrapped(y - j, n_y), core)]
                sent(came, came, s2.at[j, k], r2.at[j, k], other).wait_recv()
                across(k, j, core).start()
            return carry

        lax.fori_loop(jnp.maximum(i * per, 1), i * per + per, body, 0)

    def hop_three(i):
        def body(k, carry):
            for j in range(n_y):
                across(k, j, 1 - core).wait_recv()
            return carry

        lax.fori_loop(jnp.maximum(i * per, 1), i * per + per, body, 0)

    def compute(i):
        at = pl.ds(pl.multiple_of(i * per * cap, per * cap), per * cap)
        taken = x[at, :]
        gate_pre = jnp.dot(taken, gate_v[...], preferred_element_type=f32)
        upper = jnp.dot(taken, up_v[...], preferred_element_type=f32)
        hidden = (gate_pre / (1.0 + jnp.exp(-gate_pre)) * upper).astype(bf16)
        partial[at, :] = jnp.dot(hidden, down_v[...], preferred_element_type=f32).astype(bf16)

    def side(k):
        far = pl.ds(pl.multiple_of((1 - core) * half, half), half)
        return sent(partial.at[rows(k), far], recv_a.at[rows(k)], sa.at[k], ra.at[k], other)

    def lane(k, j):
        return sent(
            send_b.at[j, rows(k)], recv_b.at[j, rows(k)], sb.at[j, k], rb.at[j, k], along_tp(j)
        )

    def home(k):
        return sent(
            send_c.at[rows(k)], recv_c.at[rows(me)], s4.at[k], r4.at[k], {"sp": peer(k, -1)}
        )

    def pair_sum(i):
        def start(k, carry):
            side(k).start()
            return carry

        lax.fori_loop(i * per, i * per + per, start, 0)

    def lane_sum(i):
        def body(k, carry):
            side(k).wait_recv()
            for j in range(1, n_y):
                y_to = wrapped(y + j, n_y)
                send_b[j, rows(k), :] = (
                    partial[rows(k), cols(y_to, core)].astype(f32)
                    + recv_a[rows(k), sub(y_to)].astype(f32)
                ).astype(bf16)
                lane(k, j).start()
            return carry

        lax.fori_loop(i * per, i * per + per, body, 0)

    def total(k):
        summed = partial[rows(k), own].astype(f32) + recv_a[rows(k), sub(y)].astype(f32)
        for j in range(1, n_y):
            lane(k, j).wait_recv()
            summed = summed + recv_b[j, rows(k), :].astype(f32)
        return summed.astype(bf16)

    def go_home(i):
        def body(k, carry):
            send_c[rows(k), :] = total(k)
            home(k).start()
            return carry

        lax.fori_loop(jnp.maximum(i * per, 1), i * per + per, body, 0)

    hop_one(0)
    hop_two(0)
    for load in loads:
        load.wait()

    def stage(i, carry):
        hop_one(i + 1)
        hop_three(i)
        compute(i)
        pair_sum(i)
        hop_two(i + 1)

        @pl.when(i >= 1)
        def _():
            go_home(i - 1)

        lane_sum(i)
        return carry

    lax.fori_loop(0, chunks - 1, stage, 0)
    hop_three(chunks - 1)
    compute(chunks - 1)
    pair_sum(chunks - 1)
    if chunks > 1:
        go_home(chunks - 2)
    lane_sum(chunks - 1)
    recv_c[rows(me), :] = total(0)
    go_home(chunks - 1)

    def finish_home(k, carry):
        came = recv_c.at[rows(peer(k, 1))]
        sent(came, came, s4.at[k], r4.at[k], other).wait_recv()
        return carry

    lax.fori_loop(1, n_sp, finish_home, 0)
    routed[:, own] = (
        jnp.dot(mix_hi[...], recv_c[...], preferred_element_type=f32)
        + jnp.dot(mix_lo[...], recv_c[...], preferred_element_type=f32)
    ).astype(bf16)
    spread(n_y, y, core, lambda a, b: routed.at[:, cols(a, b)], (sy, ry, sc, rc))
    step = 64

    def norm(i, carry):
        at = pl.ds(pl.multiple_of(i * step, step), step)
        summed = alpha_res * normed[at, :].astype(f32) + routed[at, :].astype(f32)
        out[at, :] = layer_norm(summed, gain[...]).astype(bf16)
        return carry

    lax.fori_loop(0, out.shape[0] // step, norm, 0)

    def finish_sides(k, carry):
        side(k).wait_send()
        for j in range(1, n_y):
            lane(k, j).wait_send()
        return carry

    lax.fori_loop(0, n_sp, finish_sides, 0)

    def finish(k, carry):
        first(k).wait_send()
        home(k).wait_send()
        for j in range(n_y):
            across(k, j, core).wait_send()
        for j in range(1, n_y):
            along(k, j).wait_send()
        return carry

    lax.fori_loop(1, n_sp, finish, 0)


def called(kernel, args, shape, scratch, number, far=()):
    return pl.pallas_call(
        kernel,
        out_shape=jax.ShapeDtypeStruct(shape, bf16),
        in_specs=[
            pl.BlockSpec(memory_space=pl.ANY if n in far else pltpu.VMEM)
            for n in range(len(args))
        ],
        out_specs=pl.BlockSpec(memory_space=pltpu.VMEM),
        scratch_shapes=scratch,
        compiler_params=pltpu.CompilerParams(
            collective_id=number, has_side_effects=True, vmem_limit_bytes=60 * 1024 * 1024
        ),
    )(*args)


def spread_sems(n_y):
    return [DMA((n_y,))] * 4


def project(proj, residual, gain, n_tp):
    rows, features = proj.shape
    n_y, share = n_tp // 2, rows // n_tp
    piece = pltpu.VMEM((n_y, share, features), bf16)
    return called(
        functools.partial(project_kernel, n_tp),
        (proj, residual, gain.reshape(1, features)),
        (rows, features),
        [piece] * 3 + [DMA((n_y,))] * 4 + spread_sems(n_y),
        0,
    )


def expert_layer(select, normed, w_gate, w_up, w_down, mix_hi, mix_lo, gain, n_sp, n_tp):
    slots, (rows, features) = select.shape[0], normed.shape
    n_y, width = n_tp // 2, features // n_tp
    return called(
        functools.partial(experts_kernel, n_sp, n_tp),
        (select, normed, w_gate, w_up, w_down, mix_hi, mix_lo, gain.reshape(1, features)),
        (rows, features),
        [
            pltpu.VMEM((slots, features), bf16),
            pltpu.VMEM((slots, width), bf16),
            pltpu.VMEM(w_gate.shape[1:], bf16),
            pltpu.VMEM(w_up.shape[1:], bf16),
            pltpu.VMEM(w_down.shape[1:], bf16),
            pltpu.VMEM((slots, features), bf16),
            pltpu.VMEM((slots, features // 2), bf16),
            pltpu.VMEM((n_y, slots, width), bf16),
            pltpu.VMEM((n_y, slots, width), bf16),
            pltpu.VMEM((slots, width), bf16),
            pltpu.VMEM((slots, width), bf16),
            pltpu.VMEM((rows, features), bf16),
        ]
        + [DMA((3,))]
        + [DMA((n_sp,))] * 2
        + [DMA((n_y, n_sp))] * 4
        + [DMA((n_sp,))] * 2
        + [DMA((n_y, n_sp))] * 2
        + [DMA((n_sp,))] * 2
        + spread_sems(n_y),
        1,
        far=(2, 3, 4),
    )


def shards(
    mixer_in,
    doc_ids,
    mix_scale,
    out_proj,
    residual,
    mix_gain,
    expert_ids,
    expert_weight,
    w_gate,
    w_up,
    w_down,
    out_gain,
):
    tok_rows, chan_cols = mixer_in.shape
    features = mix_gain.shape[0]
    tail_rows = (mixer_in[tok_rows - pool_reach :], doc_ids[tok_rows - pool_reach :])
    before_vals, before_doc = passed_along((tail_rows[0], tail_rows[1]), "sp", 1)
    extended = jnp.concatenate([before_vals, mixer_in], axis=0).astype(jnp.float32)
    extended_doc = jnp.concatenate([before_doc, doc_ids], axis=0)
    positions = lax.axis_index("sp") * tok_rows + jnp.arange(tok_rows, dtype=jnp.int32)
    channel = lax.axis_index("tp") * chan_cols + jnp.arange(chan_cols, dtype=jnp.int32)
    window = jnp.left_shift(jnp.int32(2), channel // (features // 4))
    window_sum = jnp.zeros((tok_rows, chan_cols), jnp.float32)
    window_count = jnp.zeros((tok_rows, chan_cols), jnp.float32)
    for lag_step in range(pool_reach + 1):
        shifted = extended[pool_reach - lag_step : pool_reach - lag_step + tok_rows]
        same_doc = (
            extended_doc[pool_reach - lag_step : pool_reach - lag_step + tok_rows] == doc_ids
        ) & (positions >= lag_step)
        in_window = (same_doc[:, None] & (lag_step < window)[None, :]).astype(jnp.float32)
        window_sum = window_sum + in_window * shifted
        window_count = window_count + in_window
    mixed_rows = ((window_sum / window_count - extended[pool_reach:]) * mix_scale).astype(
        jnp.bfloat16
    )
    n_sp, n_tp = lax.axis_size("sp"), lax.axis_size("tp")
    product = jnp.dot(mixed_rows, out_proj, preferred_element_type=f32).astype(bf16)
    experts = n_sp
    capacity = 4 * tok_rows // experts
    ranks = pair_slots(expert_ids, experts)
    target = expert_ids * capacity + ranks
    slot_ids = jnp.arange(experts * capacity, dtype=jnp.int32)
    select = (
        (target[None, :, 0] == slot_ids[:, None]) | (target[None, :, 1] == slot_ids[:, None])
    ).astype(bf16)
    mix = jnp.sum(
        jnp.where(target[:, :, None] == slot_ids[None, None, :], expert_weight[:, :, None], 0.0),
        axis=1,
    )
    mix_hi = lax.reduce_precision(mix, 8, 7)
    mix_lo = (mix - mix_hi).astype(bf16)
    mix_hi = mix_hi.astype(bf16)
    normed = project(product, residual, mix_gain, n_tp)
    return expert_layer(
        select, normed, w_gate, w_up, w_down, mix_hi, mix_lo, out_gain, n_sp, n_tp
    )


def solution(mesh):
    placed = (
        P("sp", "tp"),
        P("sp"),
        P("tp"),
        P("tp", None),
        P("sp", None),
        P(),
        P("sp", None),
        P("sp", None),
        P("sp", None, "tp"),
        P("sp", None, "tp"),
        P("sp", "tp", None),
        P(),
    )
    return jax.shard_map(
        shards, mesh=mesh, in_specs=placed, out_specs=P("sp", None), check_vma=False
    )
```

```python
import functools

import jax
import jax.numpy as jnp
from jax import lax
from jax.experimental import pallas as pl
from jax.experimental.pallas import tpu as pltpu
from jax.sharding import PartitionSpec as P

MESH = pl.DeviceIdType.MESH
DMA = pltpu.SemaphoreType.DMA
f32 = jnp.float32
bf16 = jnp.bfloat16

alpha_res = 1.4142135623730951
norm_eps = 1e-05
pool_reach = 15


def layer_norm(summed, norm_gain):
    row_mean = jnp.mean(summed, axis=-1, keepdims=True)
    centred = summed - row_mean
    row_var = jnp.mean(centred * centred, axis=-1, keepdims=True)
    return centred * lax.rsqrt(row_var + norm_eps) * norm_gain


def wrapped(value, count):
    return lax.rem(value + 2 * count, count)


def place(n_tp):
    me = lax.axis_index("tp")
    return lax.div(me, 2), lax.rem(me, 2)


def sent(src, dst, send_sem, recv_sem, device):
    return pltpu.make_async_remote_copy(
        src_ref=src,
        dst_ref=dst,
        send_sem=send_sem,
        recv_sem=recv_sem,
        device_id=device,
        device_id_type=MESH,
    )


def greet(n_sp, n_tp):
    y, core = place(n_tp)
    n_y = n_tp // 2
    barrier = pltpu.get_barrier_semaphore()
    pl.semaphore_signal(
        barrier, inc=1, device_id={"tp": y * 2 + 1 - core}, device_id_type=MESH
    )
    for j in range(1, n_y):
        pl.semaphore_signal(
            barrier, inc=1, device_id={"tp": wrapped(y + j, n_y) * 2 + core}, device_id_type=MESH
        )
    if n_sp > 1:
        me = lax.axis_index("sp")

        def tell(k, carry):
            pl.semaphore_signal(
                barrier, inc=1, device_id={"sp": wrapped(me + k, n_sp)}, device_id_type=MESH
            )
            return carry

        lax.fori_loop(1, n_sp, tell, 0)
    pl.semaphore_wait(barrier, n_y + n_sp - 1)


def spread(n_y, y, core, part, sems):
    send_y, recv_y, send_c, recv_c = sems
    other = {"tp": y * 2 + 1 - core}
    own = part(y, core)
    along = []
    for j in range(1, n_y):
        copy = sent(
            own, own, send_y.at[j], recv_y.at[j], {"tp": wrapped(y + j, n_y) * 2 + core}
        )
        copy.start()
        along.append(copy)
    across = [sent(own, own, send_c.at[0], recv_c.at[0], other)]
    across[0].start()
    for j in range(1, n_y):
        came = part(wrapped(y - j, n_y), core)
        sent(came, came, send_y.at[j], recv_y.at[j], other).wait_recv()
        copy = sent(came, came, send_c.at[j], recv_c.at[j], other)
        copy.start()
        across.append(copy)
    for j in range(n_y):
        came = part(wrapped(y - j, n_y), 1 - core)
        sent(came, came, send_c.at[j], recv_c.at[j], other).wait_recv()
    for copy in along + across:
        copy.wait_send()


def pooled(n_sp, mixer, doc, scale, halo, halo_doc, ext, ext_doc, features):
    tok_rows, chan_cols = mixer.shape
    reach = pool_reach + 1
    ext[pl.ds(0, reach), :] = halo[...].astype(f32)
    ext[pl.ds(reach, tok_rows), :] = mixer[...].astype(f32)
    ext_doc[pl.ds(0, reach), :] = halo_doc[...]
    ext_doc[pl.ds(reach, tok_rows), :] = doc[...]
    lanes = doc.shape[1]
    position = lax.axis_index("sp") * tok_rows + lax.broadcasted_iota(
        jnp.int32, (tok_rows, lanes), 0
    )
    length = jnp.ones((tok_rows, lanes), f32)
    for lag in range(1, reach):
        same = (ext_doc[pl.ds(reach - lag, tok_rows), :] == doc[...]) & (position >= lag)
        length = length + jnp.where(same, 1.0, 0.0)
    parts = []
    for start in range(0, chan_cols, lanes):
        at = pl.ds(start, lanes)
        channel = lax.axis_index("tp") * chan_cols + start
        channel = channel + lax.broadcasted_iota(jnp.int32, (1, lanes), 1)
        window = jnp.where(channel < features // 4, 2.0, 4.0)
        window = jnp.where(channel < features // 2, window, 8.0)
        window = jnp.where(channel < features // 4 * 3, window, 16.0)
        count = jnp.minimum(window, length)
        own = ext[pl.ds(reach, tok_rows), at]
        summed = own
        for lag in range(1, reach):
            shifted = ext[pl.ds(reach - lag, tok_rows), at]
            summed = summed + jnp.where(count > lag, shifted, 0.0)
        parts.append(((summed / count - own) * scale[:, start : start + lanes]).astype(bf16))
    return jnp.concatenate(parts, axis=1) if len(parts) > 1 else parts[0]


def over_slots(mix, rows):
    return lax.dot_general(mix, rows, (((0,), (0,)), ((), ())), preferred_element_type=f32)


def tables(ids, weights, select, mix_hi, mix_lo, experts):
    tok_rows = ids.shape[1]
    cap = select.shape[0] // experts
    name = lax.broadcasted_iota(jnp.int32, (experts, tok_rows), 0)
    zero_hot, one_hot = name == ids[0:1, :], name == ids[1:2, :]
    hot = jnp.where(zero_hot | one_hot, 1.0, 0.0)
    earlier = jnp.where(
        lax.broadcasted_iota(jnp.int32, (tok_rows, tok_rows), 0)
        < lax.broadcasted_iota(jnp.int32, (tok_rows, tok_rows), 1),
        1.0,
        0.0,
    ).astype(bf16)
    rank = jnp.dot(hot.astype(bf16), earlier, preferred_element_type=f32)
    rank = jnp.where(hot > 0.0, rank, -1.0)
    share = jnp.where(zero_hot, weights[0:1, :], jnp.where(one_hot, weights[1:2, :], 0.0))
    high = share.astype(bf16).astype(f32)
    low = share - high
    slot = lax.broadcasted_iota(jnp.int32, (cap, tok_rows), 0).astype(f32)
    for e in range(experts):
        at = pl.ds(e * cap, cap)
        same = slot == rank[e : e + 1, :]
        select[at, :] = jnp.where(same, 1.0, 0.0).astype(bf16)
        mix_hi[at, :] = jnp.where(same, high[e : e + 1, :], 0.0).astype(bf16)
        mix_lo[at, :] = jnp.where(same, low[e : e + 1, :], 0.0).astype(bf16)


def layer_kernel(
    n_sp, n_tp, mixer, doc, scale, out_proj, residual, mix_gain, ids, weights,
    w_gate, w_up, w_down, gain, out,
    halo, halo_doc, ext, ext_doc, mixed, proj, half_in, half_out, share_in,
    normed, select, mix_hi, mix_lo,
    x, send, gate_v, up_v, down_v, partial, recv_a, send_b, recv_b, send_c, recv_c, routed,
    sh, rh, pa, qa, pb, qb, py, qy, pc, qc,
    sw, s1, r1, s2, r2, s3, r3, sa, ra, sb, rb, s4, r4, sy, ry, sc, rc,
):
    y, core = place(n_tp)
    n_y = n_tp // 2
    me = lax.axis_index("sp")
    cap = select.shape[0] // n_sp
    features = normed.shape[1]
    width, half = features // n_tp, features // 2
    per = max(1, min(n_sp, 256 // cap))
    chunks = n_sp // per
    other = {"tp": y * 2 + 1 - core}

    def peer(k, sign):
        outer = wrapped(lax.div(me, 2) + sign * lax.div(k, 2), n_sp // 2)
        return outer * 2 + wrapped(lax.rem(me, 2) + sign * lax.rem(k, 2), 2)

    def cols(y_of, core_of):
        return pl.ds(pl.multiple_of((core_of * n_y + y_of) * width, width), width)

    def sub(y_of):
        return pl.ds(pl.multiple_of(y_of * width, width), width)

    def rows(block):
        return pl.ds(pl.multiple_of(block * cap, cap), cap)

    def along_tp(j):
        return {"tp": wrapped(y + j, n_y) * 2 + core}

    own = cols(y, core)
    loads = [
        pltpu.make_async_copy(source.at[0], held, sw.at[n])
        for n, (source, held) in enumerate(((w_gate, gate_v), (w_up, up_v), (w_down, down_v)))
    ]
    for load in loads:
        load.start()
    greet(n_sp, n_tp)

    tok_rows = mixer.shape[0]
    reach = pool_reach + 1
    last = pl.ds(tok_rows - reach, reach)
    onward = {"sp": wrapped(me + 1, n_sp)}
    halos = [
        sent(mixer.at[last], halo, sh.at[0], rh.at[0], onward),
        sent(doc.at[last], halo_doc, sh.at[1], rh.at[1], onward),
    ]
    for copy in halos:
        copy.start()
    tables(ids, weights, select, mix_hi, mix_lo, n_sp)
    for copy in halos:
        copy.wait_recv()
    mixed[...] = pooled(n_sp, mixer, doc, scale, halo, halo_doc, ext, ext_doc, features)

    share = tok_rows // n_tp

    def held(y_of, core_of):
        return pl.ds(pl.multiple_of((core_of * n_y + y_of) * share, share), share)

    def multiply(core_of):
        at = pl.ds(pl.multiple_of(core_of * (tok_rows // 2), tok_rows // 2), tok_rows // 2)
        proj[at, :] = jnp.dot(
            mixed[at, :], out_proj[...], preferred_element_type=f32
        ).astype(bf16)

    multiply(1 - core)
    halves = {}
    for j in list(range(1, n_y)) + [0]:
        halves[j] = sent(
            proj.at[held(wrapped(y + j, n_y), 1 - core)], half_in.at[j], pa.at[j], qa.at[j], other
        )
        halves[j].start()
    multiply(core)
    shares = []
    for j in range(1, n_y):
        halves[j].wait_recv()
        half_out[j] = (
            proj[held(wrapped(y + j, n_y), core), :].astype(f32) + half_in[j].astype(f32)
        ).astype(bf16)
        copy = sent(half_out.at[j], share_in.at[j], pb.at[j], qb.at[j], along_tp(j))
        copy.start()
        shares.append(copy)
    halves[0].wait_recv()
    projected = proj[held(y, core), :].astype(f32) + half_in[0].astype(f32)
    projected = projected + alpha_res * residual[held(y, core), :].astype(f32)
    for j in range(1, n_y):
        shares[j - 1].wait_recv()
        projected = projected + share_in[j].astype(f32)
    normed[held(y, core), :] = layer_norm(projected, mix_gain[...]).astype(bf16)
    spread(n_y, y, core, lambda a, b: normed.at[held(a, b)], (py, qy, pc, qc))
    for copy in list(halves.values()) + shares + halos:
        copy.wait_send()

    def first(k):
        to = peer(k, 1)
        return sent(send.at[rows(k)], x.at[rows(k), own], s1.at[k], r1.at[k], {"sp": to})

    def along(k, j):
        piece = x.at[rows(k), own]
        return sent(piece, piece, s2.at[j, k], r2.at[j, k], along_tp(j))

    def across(k, j, core_of):
        piece = x.at[rows(k), cols(wrapped(y - j, n_y), core_of)]
        return sent(piece, piece, s3.at[j, k], r3.at[j, k], other)

    def start_first(k, carry):
        send[rows(k), :] = jnp.dot(
            select[rows(peer(k, 1)), :], normed[:, own], preferred_element_type=f32
        ).astype(bf16)
        first(k).start()
        return carry

    lax.fori_loop(1, n_sp, start_first, 0)
    x[rows(0), :] = jnp.dot(
        select[rows(me), :], normed[...], preferred_element_type=f32
    ).astype(bf16)

    def hop_one(i):
        def body(k, carry):
            first(k).wait_recv()
            for j in range(1, n_y):
                along(k, j).start()
            across(k, 0, core).start()
            return carry

        lax.fori_loop(jnp.maximum(i * per, 1), i * per + per, body, 0)

    def hop_two(i):
        def body(k, carry):
            for j in range(1, n_y):
                came = x.at[rows(k), cols(wrapped(y - j, n_y), core)]
                sent(came, came, s2.at[j, k], r2.at[j, k], other).wait_recv()
                across(k, j, core).start()
            return carry

        lax.fori_loop(jnp.maximum(i * per, 1), i * per + per, body, 0)

    def hop_three(i):
        def body(k, carry):
            for j in range(n_y):
                across(k, j, 1 - core).wait_recv()
            return carry

        lax.fori_loop(jnp.maximum(i * per, 1), i * per + per, body, 0)

    def compute(i):
        at = pl.ds(pl.multiple_of(i * per * cap, per * cap), per * cap)
        taken = x[at, :]
        gate_pre = jnp.dot(taken, gate_v[...], preferred_element_type=f32)
        upper = jnp.dot(taken, up_v[...], preferred_element_type=f32)
        hidden = (gate_pre / (1.0 + jnp.exp(-gate_pre)) * upper).astype(bf16)
        partial[at, :] = jnp.dot(hidden, down_v[...], preferred_element_type=f32).astype(bf16)

    def side(k):
        far = pl.ds(pl.multiple_of((1 - core) * half, half), half)
        return sent(partial.at[rows(k), far], recv_a.at[rows(k)], sa.at[k], ra.at[k], other)

    def lane(k, j):
        return sent(
            send_b.at[j, rows(k)], recv_b.at[j, rows(k)], sb.at[j, k], rb.at[j, k], along_tp(j)
        )

    def home(k):
        return sent(
            send_c.at[rows(k)], recv_c.at[rows(me)], s4.at[k], r4.at[k], {"sp": peer(k, -1)}
        )

    def pair_sum(i):
        def start(k, carry):
            side(k).start()
            return carry

        lax.fori_loop(i * per, i * per + per, start, 0)

    def lane_sum(i):
        def body(k, carry):
            side(k).wait_recv()
            for j in range(1, n_y):
                y_to = wrapped(y + j, n_y)
                send_b[j, rows(k), :] = (
                    partial[rows(k), cols(y_to, core)].astype(f32)
                    + recv_a[rows(k), sub(y_to)].astype(f32)
                ).astype(bf16)
                lane(k, j).start()
            return carry

        lax.fori_loop(i * per, i * per + per, body, 0)

    def total(k):
        summed = partial[rows(k), own].astype(f32) + recv_a[rows(k), sub(y)].astype(f32)
        for j in range(1, n_y):
            lane(k, j).wait_recv()
            summed = summed + recv_b[j, rows(k), :].astype(f32)
        return summed.astype(bf16)

    def go_home(i):
        def body(k, carry):
            send_c[rows(k), :] = total(k)
            home(k).start()
            return carry

        lax.fori_loop(jnp.maximum(i * per, 1), i * per + per, body, 0)

    hop_one(0)
    hop_two(0)
    for load in loads:
        load.wait()

    def stage(i, carry):
        hop_one(i + 1)
        hop_three(i)
        compute(i)
        pair_sum(i)
        hop_two(i + 1)

        @pl.when(i >= 1)
        def _():
            go_home(i - 1)

        lane_sum(i)
        return carry

    lax.fori_loop(0, chunks - 1, stage, 0)
    hop_three(chunks - 1)
    compute(chunks - 1)
    pair_sum(chunks - 1)
    if chunks > 1:
        go_home(chunks - 2)
    lane_sum(chunks - 1)
    recv_c[rows(me), :] = total(0)
    go_home(chunks - 1)

    def finish_home(k, carry):
        came = recv_c.at[rows(peer(k, 1))]
        sent(came, came, s4.at[k], r4.at[k], other).wait_recv()
        return carry

    lax.fori_loop(1, n_sp, finish_home, 0)
    routed[:, own] = (
        over_slots(mix_hi[...], recv_c[...]) + over_slots(mix_lo[...], recv_c[...])
    ).astype(bf16)
    spread(n_y, y, core, lambda a, b: routed.at[:, cols(a, b)], (sy, ry, sc, rc))
    step = 64

    def norm(i, carry):
        at = pl.ds(pl.multiple_of(i * step, step), step)
        summed = alpha_res * normed[at, :].astype(f32) + routed[at, :].astype(f32)
        out[at, :] = layer_norm(summed, gain[...]).astype(bf16)
        return carry

    lax.fori_loop(0, out.shape[0] // step, norm, 0)

    def finish_sides(k, carry):
        side(k).wait_send()
        for j in range(1, n_y):
            lane(k, j).wait_send()
        return carry

    lax.fori_loop(0, n_sp, finish_sides, 0)

    def finish(k, carry):
        first(k).wait_send()
        home(k).wait_send()
        for j in range(n_y):
            across(k, j, core).wait_send()
        for j in range(1, n_y):
            along(k, j).wait_send()
        return carry

    lax.fori_loop(1, n_sp, finish, 0)


def called(kernel, args, shape, scratch, number, far=()):
    return pl.pallas_call(
        kernel,
        out_shape=jax.ShapeDtypeStruct(shape, bf16),
        in_specs=[
            pl.BlockSpec(memory_space=pl.ANY if n in far else pltpu.VMEM)
            for n in range(len(args))
        ],
        out_specs=pl.BlockSpec(memory_space=pltpu.VMEM),
        scratch_shapes=scratch,
        compiler_params=pltpu.CompilerParams(
            collective_id=number, has_side_effects=True, vmem_limit_bytes=60 * 1024 * 1024
        ),
    )(*args)


def spread_sems(n_y):
    return [DMA((n_y,))] * 4


def shards(
    mixer_in,
    doc_ids,
    mix_scale,
    out_proj,
    residual,
    mix_gain,
    expert_ids,
    expert_weight,
    w_gate,
    w_up,
    w_down,
    out_gain,
):
    n_sp, n_tp = lax.axis_size("sp"), lax.axis_size("tp")
    n_y = n_tp // 2
    rows, chan_cols = mixer_in.shape
    features = mix_gain.shape[0]
    width = features // n_tp
    slots = 4 * rows // n_sp * n_sp
    reach = pool_reach + 1
    lanes = 128

    def vmem(*shape):
        return pltpu.VMEM(shape, bf16)

    return called(
        functools.partial(layer_kernel, n_sp, n_tp),
        (
            mixer_in,
            jnp.broadcast_to(doc_ids[:, None], (rows, lanes)),
            mix_scale.reshape(1, chan_cols),
            out_proj,
            residual,
            mix_gain.reshape(1, features),
            expert_ids.T,
            expert_weight.T,
            w_gate,
            w_up,
            w_down,
            out_gain.reshape(1, features),
        ),
        (rows, features),
        [
            vmem(reach, chan_cols),
            pltpu.VMEM((reach, lanes), jnp.int32),
            pltpu.VMEM((rows + reach, chan_cols), f32),
            pltpu.VMEM((rows + reach, lanes), jnp.int32),
            vmem(rows, chan_cols),
            vmem(rows, features),
            vmem(n_y, rows // n_tp, features),
            vmem(n_y, rows // n_tp, features),
            vmem(n_y, rows // n_tp, features),
            vmem(rows, features),
            vmem(slots, rows),
            vmem(slots, rows),
            vmem(slots, rows),
            vmem(slots, features),
            vmem(slots, width),
            vmem(*w_gate.shape[1:]),
            vmem(*w_up.shape[1:]),
            vmem(*w_down.shape[1:]),
            vmem(slots, features),
            vmem(slots, features // 2),
            vmem(n_y, slots, width),
            vmem(n_y, slots, width),
            vmem(slots, width),
            vmem(slots, width),
            vmem(rows, features),
        ]
        + [DMA((2,))] * 2
        + [DMA((n_y,))] * 4
        + spread_sems(n_y)
        + [DMA((3,))]
        + [DMA((n_sp,))] * 2
        + [DMA((n_y, n_sp))] * 4
        + [DMA((n_sp,))] * 2
        + [DMA((n_y, n_sp))] * 2
        + [DMA((n_sp,))] * 2
        + spread_sems(n_y),
        0,
        far=(8, 9, 10),
    )


def solution(mesh):
    placed = (
        P("sp", "tp"),
        P("sp"),
        P("tp"),
        P("tp", None),
        P("sp", None),
        P(),
        P("sp", None),
        P("sp", None),
        P("sp", None, "tp"),
        P("sp", None, "tp"),
        P("sp", "tp", None),
        P(),
    )
    return jax.shard_map(
        shards, mesh=mesh, in_specs=placed, out_specs=P("sp", None), check_vma=False
    )
```

```python
import functools

import jax
import jax.numpy as jnp
from jax import lax
from jax.experimental import pallas as pl
from jax.experimental.pallas import tpu as pltpu
from jax.sharding import PartitionSpec as P

MESH = pl.DeviceIdType.MESH
DMA = pltpu.SemaphoreType.DMA
f32 = jnp.float32
bf16 = jnp.bfloat16

alpha_res = 1.4142135623730951
norm_eps = 1e-05
pool_reach = 15


def layer_norm(summed, norm_gain):
    row_mean = jnp.mean(summed, axis=-1, keepdims=True)
    centred = summed - row_mean
    row_var = jnp.mean(centred * centred, axis=-1, keepdims=True)
    return centred * lax.rsqrt(row_var + norm_eps) * norm_gain


def wrapped(value, count):
    return lax.rem(value + 2 * count, count)


def place(n_tp):
    me = lax.axis_index("tp")
    return lax.div(me, 2), lax.rem(me, 2)


def sent(src, dst, send_sem, recv_sem, device):
    return pltpu.make_async_remote_copy(
        src_ref=src,
        dst_ref=dst,
        send_sem=send_sem,
        recv_sem=recv_sem,
        device_id=device,
        device_id_type=MESH,
    )


def greet(n_sp, n_tp):
    y, core = place(n_tp)
    n_y = n_tp // 2
    barrier = pltpu.get_barrier_semaphore()
    pl.semaphore_signal(
        barrier, inc=1, device_id={"tp": y * 2 + 1 - core}, device_id_type=MESH
    )
    for j in range(1, n_y):
        pl.semaphore_signal(
            barrier, inc=1, device_id={"tp": wrapped(y + j, n_y) * 2 + core}, device_id_type=MESH
        )
    if n_sp > 1:
        me = lax.axis_index("sp")

        def tell(k, carry):
            pl.semaphore_signal(
                barrier, inc=1, device_id={"sp": wrapped(me + k, n_sp)}, device_id_type=MESH
            )
            return carry

        lax.fori_loop(1, n_sp, tell, 0)
    pl.semaphore_wait(barrier, n_y + n_sp - 1)


def spread(n_y, y, core, part, sems):
    send_y, recv_y, send_c, recv_c = sems
    other = {"tp": y * 2 + 1 - core}
    own = part(y, core)
    along = []
    for j in range(1, n_y):
        copy = sent(
            own, own, send_y.at[j], recv_y.at[j], {"tp": wrapped(y + j, n_y) * 2 + core}
        )
        copy.start()
        along.append(copy)
    across = [sent(own, own, send_c.at[0], recv_c.at[0], other)]
    across[0].start()
    for j in range(1, n_y):
        came = part(wrapped(y - j, n_y), core)
        sent(came, came, send_y.at[j], recv_y.at[j], other).wait_recv()
        copy = sent(came, came, send_c.at[j], recv_c.at[j], other)
        copy.start()
        across.append(copy)
    for j in range(n_y):
        came = part(wrapped(y - j, n_y), 1 - core)
        sent(came, came, send_c.at[j], recv_c.at[j], other).wait_recv()
    for copy in along + across:
        copy.wait_send()


def pooled(n_sp, mixer, doc, scale, halo, halo_doc, ext, ext_doc, features):
    tok_rows, chan_cols = mixer.shape
    reach = pool_reach + 1
    ext[pl.ds(0, reach), :] = halo[...].astype(f32)
    ext[pl.ds(reach, tok_rows), :] = mixer[...].astype(f32)
    ext_doc[pl.ds(0, reach), :] = halo_doc[...]
    ext_doc[pl.ds(reach, tok_rows), :] = doc[...]
    lanes = doc.shape[1]
    position = lax.axis_index("sp") * tok_rows + lax.broadcasted_iota(
        jnp.int32, (tok_rows, lanes), 0
    )
    length = jnp.ones((tok_rows, lanes), f32)
    for lag in range(1, reach):
        same = (ext_doc[pl.ds(reach - lag, tok_rows), :] == doc[...]) & (position >= lag)
        length = length + jnp.where(same, 1.0, 0.0)
    parts = []
    for start in range(0, chan_cols, lanes):
        at = pl.ds(start, lanes)
        channel = lax.axis_index("tp") * chan_cols + start
        channel = channel + lax.broadcasted_iota(jnp.int32, (1, lanes), 1)
        window = jnp.where(channel < features // 4, 2.0, 4.0)
        window = jnp.where(channel < features // 2, window, 8.0)
        window = jnp.where(channel < features // 4 * 3, window, 16.0)
        count = jnp.minimum(window, length)
        own = ext[pl.ds(reach, tok_rows), at]
        summed = own
        for lag in range(1, reach):
            shifted = ext[pl.ds(reach - lag, tok_rows), at]
            summed = summed + jnp.where(count > lag, shifted, 0.0)
        parts.append(((summed / count - own) * scale[:, start : start + lanes]).astype(bf16))
    return jnp.concatenate(parts, axis=1) if len(parts) > 1 else parts[0]


def over_slots(mix, rows):
    return lax.dot_general(mix, rows, (((0,), (0,)), ((), ())), preferred_element_type=f32)


def tables(ids, weights, select, mix_hi, mix_lo, experts):
    tok_rows = ids.shape[1]
    cap = select.shape[0] // experts
    name = lax.broadcasted_iota(jnp.int32, (experts, tok_rows), 0)
    zero_hot, one_hot = name == ids[0:1, :], name == ids[1:2, :]
    hot = jnp.where(zero_hot | one_hot, 1.0, 0.0)
    earlier = jnp.where(
        lax.broadcasted_iota(jnp.int32, (tok_rows, tok_rows), 0)
        < lax.broadcasted_iota(jnp.int32, (tok_rows, tok_rows), 1),
        1.0,
        0.0,
    ).astype(bf16)
    rank = jnp.dot(hot.astype(bf16), earlier, preferred_element_type=f32)
    rank = jnp.where(hot > 0.0, rank, -1.0)
    share = jnp.where(zero_hot, weights[0:1, :], jnp.where(one_hot, weights[1:2, :], 0.0))
    high = share.astype(bf16).astype(f32)
    low = share - high
    slot = lax.broadcasted_iota(jnp.int32, (cap, tok_rows), 0).astype(f32)
    for e in range(experts):
        at = pl.ds(e * cap, cap)
        same = slot == rank[e : e + 1, :]
        select[at, :] = jnp.where(same, 1.0, 0.0).astype(bf16)
        mix_hi[at, :] = jnp.where(same, high[e : e + 1, :], 0.0).astype(bf16)
        mix_lo[at, :] = jnp.where(same, low[e : e + 1, :], 0.0).astype(bf16)


def layer_kernel(
    n_sp, n_tp, mixer, doc, scale, out_proj, residual, mix_gain, ids, weights,
    w_gate, w_up, w_down, gain, out,
    halo, halo_doc, ext, ext_doc, mixed, proj, half_in, half_out, share_in,
    normed, select, mix_hi, mix_lo,
    x, send, gate_v, up_v, down_v, partial, recv_a, send_b, recv_b, send_c, recv_c, routed,
    sh, rh, pa, qa, pb, qb, py, qy, pc, qc,
    sw, s1, r1, s2, r2, s3, r3, sa, ra, sb, rb, s4, r4, sy, ry, sc, rc,
):
    y, core = place(n_tp)
    n_y = n_tp // 2
    me = lax.axis_index("sp")
    cap = select.shape[0] // n_sp
    features = normed.shape[1]
    width, half = features // n_tp, features // 2
    per = max(1, min(n_sp, 128 // cap))
    chunks = n_sp // per
    other = {"tp": y * 2 + 1 - core}

    def peer(k, sign):
        outer = wrapped(lax.div(me, 2) + sign * lax.div(k, 2), n_sp // 2)
        return outer * 2 + wrapped(lax.rem(me, 2) + sign * lax.rem(k, 2), 2)

    def cols(y_of, core_of):
        return pl.ds(pl.multiple_of((core_of * n_y + y_of) * width, width), width)

    def sub(y_of):
        return pl.ds(pl.multiple_of(y_of * width, width), width)

    def rows(block):
        return pl.ds(pl.multiple_of(block * cap, cap), cap)

    def along_tp(j):
        return {"tp": wrapped(y + j, n_y) * 2 + core}

    own = cols(y, core)
    loads = [
        pltpu.make_async_copy(source.at[0], held, sw.at[n])
        for n, (source, held) in enumerate(((w_gate, gate_v), (w_up, up_v), (w_down, down_v)))
    ]
    for load in loads:
        load.start()
    greet(n_sp, n_tp)

    tok_rows = mixer.shape[0]
    reach = pool_reach + 1
    last = pl.ds(tok_rows - reach, reach)
    onward = {"sp": wrapped(me + 1, n_sp)}
    halos = [
        sent(mixer.at[last], halo, sh.at[0], rh.at[0], onward),
        sent(doc.at[last], halo_doc, sh.at[1], rh.at[1], onward),
    ]
    for copy in halos:
        copy.start()
    tables(ids, weights, select, mix_hi, mix_lo, n_sp)
    for copy in halos:
        copy.wait_recv()
    mixed[...] = pooled(n_sp, mixer, doc, scale, halo, halo_doc, ext, ext_doc, features)

    share = tok_rows // n_tp

    def held(y_of, core_of):
        return pl.ds(pl.multiple_of((core_of * n_y + y_of) * share, share), share)

    def multiply(core_of):
        at = pl.ds(pl.multiple_of(core_of * (tok_rows // 2), tok_rows // 2), tok_rows // 2)
        proj[at, :] = jnp.dot(
            mixed[at, :], out_proj[...], preferred_element_type=f32
        ).astype(bf16)

    multiply(1 - core)
    halves = {}
    for j in list(range(1, n_y)) + [0]:
        halves[j] = sent(
            proj.at[held(wrapped(y + j, n_y), 1 - core)], half_in.at[j], pa.at[j], qa.at[j], other
        )
        halves[j].start()
    multiply(core)
    shares = []
    for j in range(1, n_y):
        halves[j].wait_recv()
        half_out[j] = (
            proj[held(wrapped(y + j, n_y), core), :].astype(f32) + half_in[j].astype(f32)
        ).astype(bf16)
        copy = sent(half_out.at[j], share_in.at[j], pb.at[j], qb.at[j], along_tp(j))
        copy.start()
        shares.append(copy)
    halves[0].wait_recv()
    projected = proj[held(y, core), :].astype(f32) + half_in[0].astype(f32)
    projected = projected + alpha_res * residual[held(y, core), :].astype(f32)
    for j in range(1, n_y):
        shares[j - 1].wait_recv()
        projected = projected + share_in[j].astype(f32)
    normed[held(y, core), :] = layer_norm(projected, mix_gain[...]).astype(bf16)
    spread(n_y, y, core, lambda a, b: normed.at[held(a, b)], (py, qy, pc, qc))
    for copy in list(halves.values()) + shares + halos:
        copy.wait_send()

    def first(k):
        to = peer(k, 1)
        return sent(send.at[rows(k)], x.at[rows(k), own], s1.at[k], r1.at[k], {"sp": to})

    def along(k, j):
        piece = x.at[rows(k), own]
        return sent(piece, piece, s2.at[j, k], r2.at[j, k], along_tp(j))

    def across(k, j, core_of):
        piece = x.at[rows(k), cols(wrapped(y - j, n_y), core_of)]
        return sent(piece, piece, s3.at[j, k], r3.at[j, k], other)

    def start_first(k, carry):
        send[rows(k), :] = jnp.dot(
            select[rows(peer(k, 1)), :], normed[:, own], preferred_element_type=f32
        ).astype(bf16)
        first(k).start()
        return carry

    lax.fori_loop(1, n_sp, start_first, 0)
    x[rows(0), :] = jnp.dot(
        select[rows(me), :], normed[...], preferred_element_type=f32
    ).astype(bf16)

    def hop_one(i):
        def body(k, carry):
            first(k).wait_recv()
            for j in range(1, n_y):
                along(k, j).start()
            across(k, 0, core).start()
            return carry

        lax.fori_loop(jnp.maximum(i * per, 1), i * per + per, body, 0)

    def hop_two(i):
        def body(k, carry):
            for j in range(1, n_y):
                came = x.at[rows(k), cols(wrapped(y - j, n_y), core)]
                sent(came, came, s2.at[j, k], r2.at[j, k], other).wait_recv()
                across(k, j, core).start()
            return carry

        lax.fori_loop(jnp.maximum(i * per, 1), i * per + per, body, 0)

    def hop_three(i):
        def body(k, carry):
            for j in range(n_y):
                across(k, j, 1 - core).wait_recv()
            return carry

        lax.fori_loop(jnp.maximum(i * per, 1), i * per + per, body, 0)

    def compute(i):
        at = pl.ds(pl.multiple_of(i * per * cap, per * cap), per * cap)
        taken = x[at, :]
        gate_pre = jnp.dot(taken, gate_v[...], preferred_element_type=f32)
        upper = jnp.dot(taken, up_v[...], preferred_element_type=f32)
        hidden = (gate_pre / (1.0 + jnp.exp(-gate_pre)) * upper).astype(bf16)
        partial[at, :] = jnp.dot(hidden, down_v[...], preferred_element_type=f32).astype(bf16)

    def side(k):
        far = pl.ds(pl.multiple_of((1 - core) * half, half), half)
        return sent(partial.at[rows(k), far], recv_a.at[rows(k)], sa.at[k], ra.at[k], other)

    def lane(k, j):
        return sent(
            send_b.at[j, rows(k)], recv_b.at[j, rows(k)], sb.at[j, k], rb.at[j, k], along_tp(j)
        )

    def home(k):
        return sent(
            send_c.at[rows(k)], recv_c.at[rows(me)], s4.at[k], r4.at[k], {"sp": peer(k, -1)}
        )

    def pair_sum(i):
        def start(k, carry):
            side(k).start()
            return carry

        lax.fori_loop(i * per, i * per + per, start, 0)

    def lane_sum(i):
        def body(k, carry):
            side(k).wait_recv()
            for j in range(1, n_y):
                y_to = wrapped(y + j, n_y)
                send_b[j, rows(k), :] = (
                    partial[rows(k), cols(y_to, core)].astype(f32)
                    + recv_a[rows(k), sub(y_to)].astype(f32)
                ).astype(bf16)
                lane(k, j).start()
            return carry

        lax.fori_loop(i * per, i * per + per, body, 0)

    def total(k):
        summed = partial[rows(k), own].astype(f32) + recv_a[rows(k), sub(y)].astype(f32)
        for j in range(1, n_y):
            lane(k, j).wait_recv()
            summed = summed + recv_b[j, rows(k), :].astype(f32)
        return summed.astype(bf16)

    def go_home(i):
        def body(k, carry):
            send_c[rows(k), :] = total(k)
            home(k).start()
            return carry

        lax.fori_loop(jnp.maximum(i * per, 1), i * per + per, body, 0)

    hop_one(0)
    hop_two(0)
    if chunks > 1:
        hop_one(1)
    for load in loads:
        load.wait()

    def stage(i, carry):
        @pl.when(i + 2 < chunks)
        def _():
            hop_one(i + 2)

        hop_three(i)
        compute(i)
        pair_sum(i)

        @pl.when(i + 1 < chunks)
        def _():
            hop_two(i + 1)

        @pl.when(i >= 2)
        def _():
            go_home(i - 2)

        lane_sum(i)
        return carry

    lax.fori_loop(0, chunks, stage, 0)
    if chunks > 1:
        go_home(chunks - 2)
    recv_c[rows(me), :] = total(0)
    go_home(chunks - 1)

    def finish_home(k, carry):
        came = recv_c.at[rows(peer(k, 1))]
        sent(came, came, s4.at[k], r4.at[k], other).wait_recv()
        return carry

    lax.fori_loop(1, n_sp, finish_home, 0)
    routed[:, own] = (
        over_slots(mix_hi[...], recv_c[...]) + over_slots(mix_lo[...], recv_c[...])
    ).astype(bf16)
    spread(n_y, y, core, lambda a, b: routed.at[:, cols(a, b)], (sy, ry, sc, rc))
    step = 64

    def norm(i, carry):
        at = pl.ds(pl.multiple_of(i * step, step), step)
        summed = alpha_res * normed[at, :].astype(f32) + routed[at, :].astype(f32)
        out[at, :] = layer_norm(summed, gain[...]).astype(bf16)
        return carry

    lax.fori_loop(0, out.shape[0] // step, norm, 0)

    def finish_sides(k, carry):
        side(k).wait_send()
        for j in range(1, n_y):
            lane(k, j).wait_send()
        return carry

    lax.fori_loop(0, n_sp, finish_sides, 0)

    def finish(k, carry):
        first(k).wait_send()
        home(k).wait_send()
        for j in range(n_y):
            across(k, j, core).wait_send()
        for j in range(1, n_y):
            along(k, j).wait_send()
        return carry

    lax.fori_loop(1, n_sp, finish, 0)


def called(kernel, args, shape, scratch, number, far=()):
    return pl.pallas_call(
        kernel,
        out_shape=jax.ShapeDtypeStruct(shape, bf16),
        in_specs=[
            pl.BlockSpec(memory_space=pl.ANY if n in far else pltpu.VMEM)
            for n in range(len(args))
        ],
        out_specs=pl.BlockSpec(memory_space=pltpu.VMEM),
        scratch_shapes=scratch,
        compiler_params=pltpu.CompilerParams(
            collective_id=number, has_side_effects=True, vmem_limit_bytes=60 * 1024 * 1024
        ),
    )(*args)


def spread_sems(n_y):
    return [DMA((n_y,))] * 4


def shards(
    mixer_in,
    doc_ids,
    mix_scale,
    out_proj,
    residual,
    mix_gain,
    expert_ids,
    expert_weight,
    w_gate,
    w_up,
    w_down,
    out_gain,
):
    n_sp, n_tp = lax.axis_size("sp"), lax.axis_size("tp")
    n_y = n_tp // 2
    rows, chan_cols = mixer_in.shape
    features = mix_gain.shape[0]
    width = features // n_tp
    slots = 4 * rows // n_sp * n_sp
    reach = pool_reach + 1
    lanes = 128

    def vmem(*shape):
        return pltpu.VMEM(shape, bf16)

    return called(
        functools.partial(layer_kernel, n_sp, n_tp),
        (
            mixer_in,
            jnp.broadcast_to(doc_ids[:, None], (rows, lanes)),
            mix_scale.reshape(1, chan_cols),
            out_proj,
            residual,
            mix_gain.reshape(1, features),
            expert_ids.T,
            expert_weight.T,
            w_gate,
            w_up,
            w_down,
            out_gain.reshape(1, features),
        ),
        (rows, features),
        [
            vmem(reach, chan_cols),
            pltpu.VMEM((reach, lanes), jnp.int32),
            pltpu.VMEM((rows + reach, chan_cols), f32),
            pltpu.VMEM((rows + reach, lanes), jnp.int32),
            vmem(rows, chan_cols),
            vmem(rows, features),
            vmem(n_y, rows // n_tp, features),
            vmem(n_y, rows // n_tp, features),
            vmem(n_y, rows // n_tp, features),
            vmem(rows, features),
            vmem(slots, rows),
            vmem(slots, rows),
            vmem(slots, rows),
            vmem(slots, features),
            vmem(slots, width),
            vmem(*w_gate.shape[1:]),
            vmem(*w_up.shape[1:]),
            vmem(*w_down.shape[1:]),
            vmem(slots, features),
            vmem(slots, features // 2),
            vmem(n_y, slots, width),
            vmem(n_y, slots, width),
            vmem(slots, width),
            vmem(slots, width),
            vmem(rows, features),
        ]
        + [DMA((2,))] * 2
        + [DMA((n_y,))] * 4
        + spread_sems(n_y)
        + [DMA((3,))]
        + [DMA((n_sp,))] * 2
        + [DMA((n_y, n_sp))] * 4
        + [DMA((n_sp,))] * 2
        + [DMA((n_y, n_sp))] * 2
        + [DMA((n_sp,))] * 2
        + spread_sems(n_y),
        0,
        far=(8, 9, 10),
    )


def solution(mesh):
    placed = (
        P("sp", "tp"),
        P("sp"),
        P("tp"),
        P("tp", None),
        P("sp", None),
        P(),
        P("sp", None),
        P("sp", None),
        P("sp", None, "tp"),
        P("sp", None, "tp"),
        P("sp", "tp", None),
        P(),
    )
    return jax.shard_map(
        shards, mesh=mesh, in_specs=placed, out_specs=P("sp", None), check_vma=False
    )
```
